32 devices in a mesh: kv: 8 (over z, x), tp: 4 (over y, core).
Axes of the slice: x: 2, y: 2, z: 4, core: 2. Of those that a mesh axis runs over, the one named last changes fastest.
Arguments:
- tokens: bfloat16 [256, 4096], P('kv', 'tp'), may hold values from -12 to 12
- norm_gain: float32 [4096], replicated, may hold values from 0.1 to 1.9
- query_weight: bfloat16 [4096, 4096], P('kv', 'tp'), may hold values from -0.09375 to 0.09375
- key_weight: bfloat16 [4096, 4096], P('kv', 'tp'), may hold values from -0.09375 to 0.09375
- value_weight: bfloat16 [4096, 4096], P('kv', 'tp'), may hold values from -0.09375 to 0.09375
- outgate_weight: bfloat16 [4096, 4096], P('kv', 'tp'), may hold values from -0.09375 to 0.09375
- ingate_weight: bfloat16 [4096, 16], replicated, may hold values from -0.09375 to 0.09375
- forget_weight: bfloat16 [4096, 16], replicated, may hold values from -0.09375 to 0.09375
- forget_bias: float32 [16], replicated, may hold values from 0.5 to 4
- output_weight: bfloat16 [4096, 4096], P('tp', 'kv'), may hold values from -0.09375 to 0.09375
- state_memory: float32 [64, 16, 256, 256], P('kv', 'tp'), may hold values from -0.8 to 0.8
- state_normaliser: float32 [64, 16, 256], P('kv', 'tp'), may hold values from -0.8 to 0.8
- state_stabiliser: float32 [64, 16], P('kv', 'tp'), may hold values from -4 to 4
- past_keys: bfloat16 [64, 4, 4096], P('kv', None, 'tp'), may hold values from -6 to 6
- past_values: bfloat16 [64, 4, 4096], P('kv', None, 'tp'), may hold values from -6 to 6
- past_ingate: float32 [64, 4, 16], P('kv', None, 'tp'), may hold values from -4 to 4
- past_forget: float32 [64, 4, 16], P('kv', None, 'tp'), may hold values from -1 to 4
- accepted: int32 [64], P('kv'), may hold values from 0 to 4
Outputs:
- mixed: bfloat16 [256, 4096], P('kv', 'tp')
- taken_memory: float32 [64, 16, 256, 256], P('kv', 'tp')
- taken_normaliser: float32 [64, 16, 256], P('kv', 'tp')
- taken_stabiliser: float32 [64, 16], P('kv', 'tp')
- new_keys: bfloat16 [256, 4096], P('kv', 'tp')
- new_values: bfloat16 [256, 4096], P('kv', 'tp')
The draws below stay inside these ranges and needn't reach their ends.
All inputs are finite; a program needn't handle non-finite values.
Results may differ from the reference program's by a relative error of at most 0.03.
Values may be sent and summed in bfloat16 or wider, within the bound.
No kernel may reach another device: no remote copies, remote signals or barrier semaphores. Data moves between devices by JAX's collectives and lax.ppermute only.
A program may use at most 64 MiB of HBM per device.

```python
import jax
import jax.numpy as jnp
from jax import lax

D = 4096
HEADS = 16
DK = 256
DV = 256
PROPS = 4
SEQS = 64
TOKENS = 256
HD = 4096
N_TP = 4


def draw_tokens(key, part):
    base_key = jax.random.fold_in(key, 11)
    scale_key = jax.random.fold_in(key, 12)
    base_values = jnp.clip(jax.random.normal(base_key, (TOKENS, D), jnp.float32), -4.0, 4.0)
    levels = jax.random.uniform(scale_key, (TOKENS, 32), jnp.float32, jnp.log(0.3), jnp.log(3.0))
    block_scale = jnp.repeat(jnp.exp(levels), D // 32, axis=1)
    return (base_values * block_scale).astype(jnp.bfloat16)


def touch_ends(array, stream_key, smallest, top_value):
    index_at = [jax.random.randint(jax.random.fold_in(stream_key, axis), (), 0, length) for axis, length in enumerate(array.shape)]
    widest = array.shape.index(max(array.shape))
    beside = index_at[:widest] + [(index_at[widest] + 1) % array.shape[widest]] + index_at[widest + 1:]
    return array.at[tuple(index_at)].set(smallest).at[tuple(beside)].set(top_value)


def level_of(rng, shape, shards, least, high):
    def one(position, parts):
        steps = jax.random.uniform(jax.random.fold_in(jax.random.fold_in(rng, 6), position), (parts,), jnp.float32, least / len(shards), high / len(shards))
        return jnp.repeat(jnp.exp(steps), shape[position] // parts).reshape((-1,) + (1,) * (len(shape) - position - 1))

    gain = one(*shards[0])
    for cut in shards[1:]:
        gain = gain * one(*cut)
    return gain


def scatter_about(rng, dims, spread, most, pieces=(), held_as=jnp.bfloat16):
    array = jax.random.normal(rng, dims, jnp.float32) * spread
    if len(pieces) > 0:
        array = level_of(rng, dims, pieces, -0.22, 0.18) * array
    return jnp.clip(array, min=-most, max=most).astype(held_as)


def setup_inputs(seed: int = 0) -> dict:
    keys = jax.random.split(jax.random.key(seed), 19)
    tokens = draw_tokens(jax.random.fold_in(keys[18], 71), 0)
    norm_gain = jnp.clip(1.0 + 0.18 * jax.random.normal(keys[1], (D,), jnp.float32), 0.1, 1.9)
    query_weight = scatter_about(keys[2], (D, HD), D ** -0.5, 0.09375, ((0, 8), (1, 4)))
    key_weight = scatter_about(keys[3], (D, HD), D ** -0.5, 0.09375, ((0, 8), (1, 4)))
    value_weight = scatter_about(keys[4], (D, HD), D ** -0.5, 0.09375, ((0, 8), (1, 4)))
    outgate_weight = scatter_about(keys[5], (D, HD), D ** -0.5, 0.09375, ((0, 8), (1, 4)))
    ingate_weight = scatter_about(keys[6], (D, HEADS), D ** -0.5, 0.09375)
    forget_weight = scatter_about(keys[7], (D, HEADS), D ** -0.5, 0.09375)
    forget_bias = jnp.clip(jax.random.uniform(keys[8], (HEADS,), jnp.float32, 0.5, 4.0), 0.5, 4.0)
    output_weight = scatter_about(keys[9], (HD, D), HD ** -0.5, 0.09375, ((0, 4), (1, 8)))
    state_memory = scatter_about(keys[10], (SEQS, HEADS, DK, DV), 0.1, 0.8, ((0, 8), (1, 4)), jnp.float32)
    state_normaliser = scatter_about(keys[11], (SEQS, HEADS, DK), 0.1, 0.8, ((0, 8), (1, 4)), jnp.float32)
    state_stabiliser = scatter_about(keys[12], (SEQS, HEADS), 1.0, 4.0, ((0, 8), (1, 4)), jnp.float32)
    past_keys = scatter_about(keys[13], (SEQS, PROPS, HD), 1.0, 6.0, ((0, 8), (2, 4)))
    past_values = scatter_about(keys[14], (SEQS, PROPS, HD), 1.0, 6.0, ((0, 8), (2, 4)))
    past_ingate = scatter_about(keys[15], (SEQS, PROPS, HEADS), 1.0, 4.0, ((0, 8), (2, 4)), jnp.float32)
    past_forget = jnp.clip(-1.0 + 5.0 * jax.random.uniform(keys[16], (SEQS, PROPS, HEADS), jnp.float32) ** level_of(keys[16], (SEQS, PROPS, HEADS), ((0, 8), (2, 4)), -0.2, 0.2), -1.0, 4.0)
    accepted = touch_ends(jax.random.randint(keys[17], (SEQS,), 0, PROPS + 1), jax.random.fold_in(keys[17], 1), 0, PROPS).astype(jnp.int32)
    return dict(tokens=tokens, norm_gain=norm_gain, query_weight=query_weight, key_weight=key_weight, value_weight=value_weight, outgate_weight=outgate_weight, ingate_weight=ingate_weight, forget_weight=forget_weight, forget_bias=forget_bias, output_weight=output_weight, state_memory=state_memory, state_normaliser=state_normaliser, state_stabiliser=state_stabiliser, past_keys=past_keys, past_values=past_values, past_ingate=past_ingate, past_forget=past_forget, accepted=accepted)


exact_mode = lax.Precision.HIGHEST
epsilon = 1e-06

def rounded(values):
    return lax.optimization_barrier(values.astype(jnp.bfloat16))

def heads_view(rows, seq_count, head_count):
    shaped = rows.astype(jnp.float32).reshape(seq_count, -1, head_count, rows.shape[-1] // head_count)
    return shaped.transpose(0, 2, 1, 3)

def catch_up(memory, normaliser, stabiliser, key_rows, values, in_gate, forget_pre, taken_mask):
    log_forget = jnp.where(taken_mask, jax.nn.log_sigmoid(forget_pre), 0.0)
    running = jnp.cumsum(log_forget, axis=-1)
    chain_total = running[..., -1]
    end_logs = jnp.where(taken_mask, chain_total[..., None] - running + in_gate, -jnp.inf)
    stable_new = jnp.maximum(chain_total + stabiliser, lax.optimization_barrier(jnp.max(end_logs, axis=-1)))
    carry_decay = jnp.exp(chain_total + stabiliser - stable_new)
    weighted = key_rows * jnp.exp(end_logs - stable_new[..., None])[..., None]
    memory_new = carry_decay[..., None, None] * memory + jnp.einsum('...pd,...pe->...de', weighted, values, precision=exact_mode)
    normaliser_new = carry_decay[..., None] * normaliser + lax.optimization_barrier(jnp.sum(weighted, axis=-2))
    return (memory_new, normaliser_new, stable_new)

def advance(memory, normaliser, stabiliser, query_rows, key_rows, values, in_gate, forget_pre):
    chain_len = query_rows.shape[-2]
    running = jnp.cumsum(jax.nn.log_sigmoid(forget_pre), axis=-1)
    causal = jnp.arange(chain_len)[:, None] >= jnp.arange(chain_len)[None, :]
    within = jnp.where(causal, running[..., :, None] - running[..., None, :] + in_gate[..., None, :], -jnp.inf)
    carried = running + stabiliser[..., None]
    stable = jnp.maximum(carried, lax.optimization_barrier(jnp.max(within, axis=-1)))
    scores = jnp.einsum('...td,...sd->...ts', query_rows, key_rows, precision=exact_mode) * jnp.exp(within - stable[..., None])
    carry_weight = jnp.exp(carried - stable)
    numerator = carry_weight[..., None] * jnp.einsum('...td,...de->...te', query_rows, memory, precision=exact_mode)
    numerator = numerator + jnp.einsum('...ts,...se->...te', scores, values, precision=exact_mode)
    denominator = carry_weight * jnp.einsum('...td,...d->...t', query_rows, normaliser, precision=exact_mode) + lax.optimization_barrier(jnp.sum(scores, axis=-1))
    return numerator / jnp.maximum(jnp.abs(denominator), 1.0)[..., None]

def reference(tokens, norm_gain, query_weight, key_weight, value_weight, outgate_weight, ingate_weight, forget_weight, forget_bias, output_weight, state_memory, state_normaliser, state_stabiliser, past_keys, past_values, past_ingate, past_forget, accepted):
    floats = tokens.astype(jnp.float32)
    squares = lax.optimization_barrier(jnp.sum(floats * floats, axis=1, keepdims=True))
    normed = (floats * lax.rsqrt(squares / D + epsilon) * norm_gain).astype(jnp.bfloat16)
    query_b = rounded(jnp.dot(normed, query_weight, preferred_element_type=jnp.float32))
    key_b = rounded(jnp.dot(normed, key_weight, preferred_element_type=jnp.float32))
    value_b = rounded(jnp.dot(normed, value_weight, preferred_element_type=jnp.float32))
    outgate_b = rounded(jnp.dot(normed, outgate_weight, preferred_element_type=jnp.float32))
    in_gate = jnp.dot(normed, ingate_weight, preferred_element_type=jnp.float32)
    forget_pre = jnp.dot(normed, forget_weight, preferred_element_type=jnp.float32) + forget_bias
    seq_count = past_keys.shape[0]
    chain_len = past_keys.shape[1]
    key_scale = DK ** (-0.5)
    query_h = heads_view(query_b, seq_count, HEADS)
    key_h = heads_view(key_b, seq_count, HEADS) * key_scale
    value_h = heads_view(value_b, seq_count, HEADS)
    outgate_h = heads_view(outgate_b, seq_count, HEADS)
    in_h = in_gate.reshape(seq_count, chain_len, HEADS).transpose(0, 2, 1)
    forget_h = forget_pre.reshape(seq_count, chain_len, HEADS).transpose(0, 2, 1)
    past_key_h = heads_view(past_keys, seq_count, HEADS) * key_scale
    past_value_h = heads_view(past_values, seq_count, HEADS)
    past_in_h = past_ingate.transpose(0, 2, 1)
    past_forget_h = past_forget.transpose(0, 2, 1)

    def per_sequence(items):
        memory, normaliser, stabiliser, query_s, key_s, value_s, outgate_s, in_s, forget_s, past_key_s, past_value_s, past_in_s, past_forget_s, taken_count = items
        taken_mask = (jnp.arange(chain_len) < taken_count)[None, :]
        memory_new, normaliser_new, stable_new = catch_up(memory, normaliser, stabiliser, past_key_s, past_value_s, past_in_s, past_forget_s, taken_mask)
        hidden = advance(memory_new, normaliser_new, stable_new, query_s, key_s, value_s, in_s, forget_s)
        gated = (jax.nn.sigmoid(outgate_s) * hidden).transpose(1, 0, 2).reshape(chain_len, -1).astype(jnp.bfloat16)
        return (memory_new, normaliser_new, stable_new, gated)
    memory_out, normaliser_out, stable_out, gated_all = lax.map(per_sequence, (state_memory, state_normaliser, state_stabiliser, query_h, key_h, value_h, outgate_h, in_h, forget_h, past_key_h, past_value_h, past_in_h, past_forget_h, accepted))
    gated_rows = gated_all.reshape(seq_count * chain_len, -1)
    groups = gated_rows.reshape(gated_rows.shape[0], N_TP, -1).transpose(1, 0, 2)
    weight_groups = output_weight.reshape(N_TP, -1, D)

    def add_group(running_sum, group_pair):
        group_sum = lax.optimization_barrier(jnp.dot(group_pair[0], group_pair[1], preferred_element_type=jnp.float32).astype(jnp.bfloat16))
        return (running_sum + group_sum.astype(jnp.float32), None)
    running_sum, ignored = lax.scan(add_group, jnp.zeros((gated_rows.shape[0], D), jnp.float32), (groups, weight_groups))
    mixed = running_sum.astype(jnp.bfloat16)
    return (mixed, memory_out, normaliser_out, stable_out, key_b, value_b)
```

```python
import functools

import jax
import jax.numpy as jnp
from jax import lax
from jax.experimental import pallas as pl
from jax.experimental.pallas import tpu as pltpu
from jax.sharding import PartitionSpec as P


EPSILON = 1e-06
LANES = 128
BOTH = ("kv", "tp")
F32 = jnp.float32
BF16 = jnp.bfloat16


def masks_of(size):
    bits = size.bit_length() - 1
    return [(2 << i) - 1 for i in range(bits)]


def spans(masks):
    found = [0]
    for mask in reversed(masks):
        found = found + [mask ^ other for other in found]
    return found


class Plan:
    def __init__(self, mesh):
        self.kv, self.tp = mesh.shape["kv"], mesh.shape["tp"]
        self.ratio = self.kv // self.tp
        assert self.ratio * self.tp == self.kv
        z_masks = [mask * self.ratio for mask in masks_of(self.tp)]
        x_masks = masks_of(self.ratio)
        self.order_a = z_masks + x_masks
        self.order_b = z_masks[::-1] + x_masks

    def pairs(self, move):
        return [
            (k * self.tp + t, move(k, t)[0] * self.tp + move(k, t)[1])
            for k in range(self.kv)
            for t in range(self.tp)
        ]

    def xor_kv(self, mask):
        return self.pairs(lambda k, t: (k ^ mask, t))

    def xor_tp(self, mask):
        return self.pairs(lambda k, t: (k, t ^ mask))

    def swap(self, mask):
        r = self.ratio
        return self.pairs(lambda k, t: (t * r + ((k % r) ^ mask), k // r))


def whole(*_):
    return pl.BlockSpec(memory_space=pltpu.VMEM)


def pack(extra):
    high = extra.astype(BF16).astype(F32)
    return high + pltpu.roll(extra - high, LANES // 2, 1)


def unpack(packed):
    lane = lax.broadcasted_iota(jnp.int32, packed.shape, 1)
    return jnp.where(lane < LANES // 2, packed + pltpu.roll(packed, LANES // 2, 1), 0.0)


def project_body(plan, block, base_ref, *refs):
    pieces = refs[: plan.tp]
    gain_ref, w0, w1, w2, w3, we = refs[plan.tp : plan.tp + 6]
    keep_a, send_a, keep_b, send_b, staged, scaled, extra = refs[plan.tp + 6 :]
    cols = w0.shape[1]
    for s, piece in enumerate(pieces):
        staged[s] = piece[...]
    base = base_ref[0]
    gain = gain_ref[...]
    rel_a = spans(plan.order_a)
    rel_b = spans(plan.order_b)
    lane = lax.broadcasted_iota(jnp.int32, (block, LANES), 1)
    for i, rel in enumerate(rel_a):
        zr, xr = rel // plan.ratio, rel % plan.ratio
        rows = staged[base ^ zr, pl.ds(xr * block, block), :].astype(F32)
        scaled[pl.ds(i * block, block), :] = (rows * gain).astype(BF16)
        squares = jnp.sum(rows * rows, axis=1, keepdims=True)
        extra[pl.ds(i * block, block), :] = jnp.where(lane == LANES // 2 - 1, squares, 0.0)
    half = len(rel_a) // 2 * block
    sums = extra[...] + jnp.dot(scaled[...], we[...], preferred_element_type=F32)
    keep_a[:, 2 * cols :] = sums[:half]
    send_a[:, 2 * cols :] = pack(sums[half:]).astype(BF16)
    for j, weight in enumerate((w0, w1)):
        out = jnp.dot(scaled[...], weight[...], preferred_element_type=F32)
        keep_a[:, j * cols : (j + 1) * cols] = out[:half]
        send_a[:, j * cols : (j + 1) * cols] = out[half:].astype(BF16)
    for j, weight in enumerate((w2, w3)):
        out = jnp.dot(scaled[...], weight[...], preferred_element_type=F32)
        for i, rel in enumerate(rel_b):
            at = rel_a.index(rel) * block
            rows = out[at : at + block]
            if i * block < half:
                keep_b[i * block : (i + 1) * block, j * cols : (j + 1) * cols] = rows
            else:
                keep = i * block - half
                send_b[keep : keep + block, j * cols : (j + 1) * cols] = rows.astype(BF16)


def project(plan, base, pieces, gain, weights, extra_weight, block):
    rows = plan.kv * block
    cols = weights[0].shape[1]
    features = pieces[0].shape[1]
    wide = 2 * cols + LANES
    return pl.pallas_call(
        functools.partial(project_body, plan, block),
        out_shape=(
            jax.ShapeDtypeStruct((rows // 2, wide), F32),
            jax.ShapeDtypeStruct((rows // 2, wide), BF16),
            jax.ShapeDtypeStruct((rows // 2, 2 * cols), F32),
            jax.ShapeDtypeStruct((rows // 2, 2 * cols), BF16),
        ),
        in_specs=[pl.BlockSpec(memory_space=pltpu.SMEM)] + [whole()] * (plan.tp + 6),
        out_specs=[whole()] * 4,
        scratch_shapes=[
            pltpu.VMEM((plan.tp, plan.ratio * block, features), BF16),
            pltpu.VMEM((rows, features), BF16),
            pltpu.VMEM((rows, LANES), F32),
        ],
        name="project",
    )(base, *pieces, gain, *weights, extra_weight)


def step_body(cols, has_extra, keep_ref, got_ref, keep_out, send_out):
    half = keep_out.shape[0]
    wide = cols * 2
    keep_out[:, :wide] = keep_ref[:half, :wide] + got_ref[:half, :wide].astype(F32)
    send_out[:, :wide] = (keep_ref[half:, :wide] + got_ref[half:, :wide].astype(F32)).astype(BF16)
    if has_extra:
        sums = keep_ref[:, wide:] + unpack(got_ref[:, wide:].astype(F32))
        keep_out[:, wide:] = sums[:half]
        send_out[:, wide:] = pack(sums[half:]).astype(BF16)


def reduce_step(cols, has_extra, keep, got):
    half, wide = keep.shape[0] // 2, keep.shape[1]
    return pl.pallas_call(
        functools.partial(step_body, cols, has_extra),
        out_shape=(
            jax.ShapeDtypeStruct((half, wide), F32),
            jax.ShapeDtypeStruct((half, wide), BF16),
        ),
        in_specs=[whole()] * 2,
        out_specs=[whole()] * 2,
        name="reduce_step",
    )(keep, got)


def state_body(decay_ref, memory_ref, key_ref, value_ref, new_ref, narrow_ref):
    seq = pl.program_id(0)
    dk = memory_ref.shape[2]
    for h in range(memory_ref.shape[1]):
        keys = key_ref[0, :, h * dk : (h + 1) * dk]
        values = value_ref[0, :, h * dk : (h + 1) * dk]
        added = lax.dot_general(keys, values, (((0,), (0,)), ((), ())), preferred_element_type=F32)
        memory = decay_ref[seq, h] * memory_ref[0, h] + added
        new_ref[0, h] = memory
        narrow_ref[0, h] = memory.astype(BF16)


def state_update(decay, memory, keys, values):
    seqs, heads, dk, dv = memory.shape
    spec = pl.BlockSpec((1, heads, dk, dv), lambda s: (s, 0, 0, 0))
    rows = pl.BlockSpec((1,) + keys.shape[1:], lambda s: (s, 0, 0))
    return pl.pallas_call(
        state_body,
        grid=(seqs,),
        out_shape=(
            jax.ShapeDtypeStruct(memory.shape, F32),
            jax.ShapeDtypeStruct(memory.shape, BF16),
        ),
        in_specs=[pl.BlockSpec(memory_space=pltpu.SMEM), spec, rows, rows],
        out_specs=[spec, spec],
        cost_estimate=pl.CostEstimate(
            flops=16 * memory.size, bytes_accessed=10 * memory.size, transcendentals=0
        ),
        name="state_update",
    )(decay, memory, keys, values)


def advance_body(
    width, chain, heads, keep_a, got_a, keep_b, got_b, memory, norm, stab, bias, gated, key_out, value_out
):
    rows = keep_a.shape[0]
    cols = gated.shape[1]
    dk = cols // heads
    extra = keep_a[:, 2 * cols :] + unpack(got_a[:, 2 * cols :].astype(F32))
    scale = lax.rsqrt(extra[:, LANES // 2 - 1 : LANES // 2] / width + EPSILON)
    gates = extra * scale
    in_gate = gates
    pre = pltpu.roll(gates, LANES - heads, 1) + bias[...]
    log_f = jax.nn.log_sigmoid(pre)
    turn = lax.broadcasted_iota(jnp.int32, (rows, LANES), 0) % chain
    running = log_f
    shift = 1
    while shift < chain:
        running = running + jnp.where(turn >= shift, pltpu.roll(running, shift, 0), 0.0)
        shift *= 2
    fresh = in_gate - running
    best = fresh
    shift = 1
    while shift < chain:
        best = jnp.maximum(best, jnp.where(turn >= shift, pltpu.roll(best, shift, 0), -jnp.inf))
        shift *= 2
    carried = running + stab[...]
    stable = jnp.maximum(carried, running + best)
    carry_weight = jnp.exp(carried - stable)
    lead = running - stable
    fresh_t = fresh.T
    at_t = lax.broadcasted_iota(jnp.int32, (rows, rows), 0)
    at_s = lax.broadcasted_iota(jnp.int32, (rows, rows), 1)
    seen = (at_t // chain == at_s // chain) & (at_s <= at_t)
    seqs = rows // chain
    seq_t = lax.broadcasted_iota(jnp.int32, (rows, seqs), 0) // chain
    seq_s = lax.broadcasted_iota(jnp.int32, (rows, seqs), 1)
    sub = 8
    sub_row = lax.broadcasted_iota(jnp.int32, (sub, dk), 0) // chain
    for h in range(heads):
        a, b = h * dk, (h + 1) * dk

        def total(keep, got, j):
            at = slice(j * cols + a, j * cols + b)
            return (keep[:, at] + got[:, at].astype(F32)) * scale

        query = total(keep_a, got_a, 0).astype(BF16)
        key = total(keep_a, got_a, 1).astype(BF16)
        value = total(keep_b, got_b, 0).astype(BF16)
        gate = total(keep_b, got_b, 1).astype(BF16).astype(F32)
        key_out[:, a:b] = key
        value_out[:, a:b] = value
        scores = lax.dot_general(query, key, (((1,), (1,)), ((), ())), preferred_element_type=F32)
        weight = jnp.exp(jnp.where(seen, lead[:, h : h + 1] + fresh_t[h : h + 1, :], -jnp.inf))
        scores = scores * (weight * dk**-0.5)
        carry = carry_weight[:, h : h + 1]
        high = scores.astype(BF16)
        low = (scores - high.astype(F32)).astype(BF16)
        inner = jnp.dot(high, value, preferred_element_type=F32) + jnp.dot(
            low, value, preferred_element_type=F32
        )
        normal = norm[:, a:b]
        n_high = normal.astype(BF16)
        n_low = (normal - n_high.astype(F32)).astype(BF16)
        dims = (((1,), (1,)), ((), ()))
        along = lax.dot_general(query, n_high, dims, preferred_element_type=F32) + lax.dot_general(
            query, n_low, dims, preferred_element_type=F32
        )
        along = jnp.sum(jnp.where(seq_t == seq_s, along, 0.0), axis=1, keepdims=True)
        below = carry * along + jnp.sum(scores, axis=1, keepdims=True)
        parts = []
        for r in range(0, rows, sub):
            part = None
            for i in range(sub // chain):
                one = jnp.dot(
                    query[r : r + sub], memory[r // chain + i, h], preferred_element_type=F32
                )
                part = one if part is None else jnp.where(sub_row == i, one, part)
            parts.append(part)
        outer = jnp.concatenate(parts, axis=0)
        hidden = (carry * outer + inner) / jnp.maximum(jnp.abs(below), 1.0)
        gated[:, a:b] = (jax.nn.sigmoid(gate) * hidden).astype(BF16)


def advance(width, chain, heads, keep_a, got_a, keep_b, got_b, memory, norm, stab, bias):
    rows = keep_a.shape[0]
    cols = keep_b.shape[1] // 2
    shape = jax.ShapeDtypeStruct((rows, cols), BF16)
    return pl.pallas_call(
        functools.partial(advance_body, width, chain, heads),
        out_shape=(shape, shape, shape),
        in_specs=[whole()] * 8,
        out_specs=[whole()] * 3,
        name="advance",
    )(keep_a, got_a, keep_b, got_b, memory, norm, stab, bias)


def output_body(plan, block, base_ref, *refs):
    pieces = refs[: plan.kv]
    weight, keep, send, staged = refs[plan.kv :]
    r, t = plan.ratio, plan.tp
    for rel, piece in enumerate(pieces):
        staged[rel // r, (rel % r) * block : (rel % r + 1) * block, :] = piece[...]
    base = base_ref[0]
    order = spans(masks_of(t))
    half = t // 2
    rows = jnp.concatenate([staged[base ^ s] for s in order], axis=0)
    out = jnp.dot(rows, weight[...], preferred_element_type=F32)
    cut = half * r * block
    keep[...] = out[:cut]
    send[...] = out[cut:].astype(BF16)


def output_product(plan, base, pieces, weight, block):
    rows = plan.kv * block // 2
    cols = weight.shape[1]
    return pl.pallas_call(
        functools.partial(output_body, plan, block),
        out_shape=(
            jax.ShapeDtypeStruct((rows, cols), F32),
            jax.ShapeDtypeStruct((rows, cols), BF16),
        ),
        in_specs=[pl.BlockSpec(memory_space=pltpu.SMEM)] + [whole()] * (plan.kv + 1),
        out_specs=[whole()] * 2,
        scratch_shapes=[pltpu.VMEM((plan.tp, plan.ratio * block, weight.shape[0]), BF16)],
        name="output_product",
    )(base, *pieces, weight)


def catch_up(stabiliser, past_in, past_forget, accepted):
    chain = past_in.shape[1]
    taken = jnp.arange(chain)[None, :, None] < accepted[:, None, None]
    log_forget = jnp.where(taken, jax.nn.log_sigmoid(past_forget), 0.0)
    rows = [log_forget[:, j] for j in range(chain)]
    total = rows[0]
    for row in rows[1:]:
        total = total + row
    run, after = None, []
    for row in rows:
        run = row if run is None else run + row
        after.append(total - run)
    ends = jnp.where(taken, jnp.stack(after, axis=1) + past_in, -jnp.inf)
    stable = jnp.maximum(total + stabiliser, jnp.max(ends, axis=1))
    decay = jnp.exp(total + stabiliser - stable)
    return stable, decay, jnp.exp(ends - stable[:, None])


def body(
    plan,
    tokens,
    norm_gain,
    query_weight,
    key_weight,
    value_weight,
    outgate_weight,
    ingate_weight,
    forget_weight,
    forget_bias,
    output_weight,
    state_memory,
    state_normaliser,
    state_stabiliser,
    past_keys,
    past_values,
    past_ingate,
    past_forget,
    accepted,
):
    seqs, heads = state_stabiliser.shape
    block, part = tokens.shape
    chain = past_keys.shape[1]
    dk = state_memory.shape[2]
    features = query_weight.shape[0]
    width = norm_gain.shape[0]
    ratio, tp = plan.ratio, plan.tp
    me, mine = lax.axis_index("kv"), lax.axis_index("tp")
    z, x = me // ratio, me % ratio
    base = (z ^ mine).astype(jnp.int32)[None]

    def pull(array, pairs):
        return lax.ppermute(array, BOTH, pairs)

    cut = tokens.reshape(block, ratio, features)
    first = [
        pull(lax.dynamic_index_in_dim(cut, x ^ m, 1, keepdims=False), plan.swap(m)) for m in range(ratio)
    ]
    own = jnp.concatenate(first, axis=0)
    pieces = [own] + [pull(own, plan.xor_tp(s)) for s in range(1, tp)]

    stable, decay, share = catch_up(state_stabiliser, past_ingate, past_forget, accepted)
    spread = jnp.repeat(share * dk**-0.5, dk, axis=2)
    weighted = past_keys.astype(F32) * spread
    high = weighted.astype(BF16)
    low = (weighted - high.astype(F32)).astype(BF16)
    memory, narrow = state_update(
        decay,
        state_memory,
        jnp.concatenate([high, low], axis=1),
        jnp.concatenate([past_values, past_values], axis=1),
    )
    normaliser = decay[..., None] * state_normaliser + jnp.sum(weighted, axis=1).reshape(seqs, heads, dk)

    gain = lax.dynamic_slice_in_dim(norm_gain, me * features, features)[None]
    gates = [
        lax.dynamic_slice(w, (me * features, mine * heads), (features, heads))
        for w in (ingate_weight, forget_weight)
    ]
    extra_weight = jnp.pad(jnp.concatenate(gates, axis=1), ((0, 0), (0, LANES - 2 * heads)))
    weights = (query_weight, key_weight, value_weight, outgate_weight)
    keep_a, send_a, keep_b, send_b = project(plan, base, pieces, gain, weights, extra_weight, block)
    cols = query_weight.shape[1]
    steps = len(plan.order_a)
    for i in range(steps):
        got_a = pull(send_a, plan.xor_kv(plan.order_a[i]))
        got_b = pull(send_b, plan.xor_kv(plan.order_b[i]))
        if i + 1 < steps:
            keep_a, send_a = reduce_step(cols, True, keep_a, got_a)
            keep_b, send_b = reduce_step(cols, False, keep_b, got_b)

    lanes = ((0, 0), (0, LANES - heads))
    stab = jnp.pad(jnp.repeat(stable, chain, axis=0), lanes)
    bias = jnp.pad(lax.dynamic_slice_in_dim(forget_bias, mine * heads, heads)[None], lanes)
    gated, new_keys, new_values = advance(
        width, chain, heads, keep_a, got_a, keep_b, got_b, narrow, normaliser.reshape(seqs, heads * dk), stab, bias
    )

    gathered = [gated] + [pull(gated, plan.xor_kv(m)) for m in range(1, plan.kv)]
    keep, send = output_product(plan, base, gathered, output_weight, block)
    for mask in masks_of(tp):
        total = keep + pull(send, plan.xor_tp(mask)).astype(F32)
        half = total.shape[0] // 2
        keep, send = total[:half], total[half:].astype(BF16)
    total = total.astype(BF16)
    back = [pull(total[m * block : (m + 1) * block], plan.swap(m)) for m in range(ratio)]
    stacked = jnp.stack(back, axis=0)
    mixed = jnp.concatenate(
        [lax.dynamic_index_in_dim(stacked, x ^ m, 0, keepdims=False) for m in range(ratio)], axis=1
    )
    return (mixed, memory, normaliser, stable, new_keys, new_values)


def solution(mesh):
    placed = (
        P("kv", "tp"),
        P(),
        P("kv", "tp"),
        P("kv", "tp"),
        P("kv", "tp"),
        P("kv", "tp"),
        P(),
        P(),
        P(),
        P("tp", "kv"),
        P("kv", "tp", None, None),
        P("kv", "tp", None),
        P("kv", "tp"),
        P("kv", None, "tp"),
        P("kv", None, "tp"),
        P("kv", None, "tp"),
        P("kv", None, "tp"),
        P("kv"),
    )
    return jax.shard_map(
        functools.partial(body, Plan(mesh)),
        mesh=mesh,
        in_specs=placed,
        out_specs=(
            P("kv", "tp"),
            P("kv", "tp", None, None),
            P("kv", "tp", None),
            P("kv", "tp"),
            P("kv", "tp"),
            P("kv", "tp"),
        ),
        check_vma=False,
    )
```

```python
import functools

import jax
import jax.numpy as jnp
from jax import lax
from jax.experimental import pallas as pl
from jax.experimental.pallas import tpu as pltpu
from jax.sharding import PartitionSpec as P


EPSILON = 1e-06
LANES = 128
BOTH = ("kv", "tp")
F32 = jnp.float32
BF16 = jnp.bfloat16


def masks_of(size):
    bits = size.bit_length() - 1
    return [(2 << i) - 1 for i in range(bits)]


def spans(masks):
    found = [0]
    for mask in reversed(masks):
        found = found + [mask ^ other for other in found]
    return found


class Plan:
    def __init__(self, mesh):
        self.kv, self.tp = mesh.shape["kv"], mesh.shape["tp"]
        self.ratio = self.kv // self.tp
        assert self.ratio * self.tp == self.kv
        z_masks = [mask * self.ratio for mask in masks_of(self.tp)]
        x_masks = masks_of(self.ratio)
        self.x_first = x_masks + z_masks
        self.z_first = z_masks + x_masks

    def pairs(self, move):
        return [
            (k * self.tp + t, move(k, t)[0] * self.tp + move(k, t)[1])
            for k in range(self.kv)
            for t in range(self.tp)
        ]

    def xor_kv(self, mask):
        return self.pairs(lambda k, t: (k ^ mask, t))

    def xor_tp(self, mask):
        return self.pairs(lambda k, t: (k, t ^ mask))

    def swap(self, mask):
        r = self.ratio
        return self.pairs(lambda k, t: (t * r + ((k % r) ^ mask), k // r))


VMEM = pl.BlockSpec(memory_space=pltpu.VMEM)
SMEM = pl.BlockSpec(memory_space=pltpu.SMEM)
UNREAD = pl.BlockSpec(memory_space=pl.ANY)


def near(array):
    return pltpu.with_memory_space_constraint(array, pltpu.VMEM)


def far(array):
    return pltpu.with_memory_space_constraint(array, pltpu.HBM)


def params(mib):
    return pltpu.CompilerParams(vmem_limit_bytes=mib << 20)


def pack(extra):
    high = extra.astype(BF16).astype(F32)
    return high + pltpu.roll(extra - high, LANES // 2, 1)


def unpack(packed):
    lane = lax.broadcasted_iota(jnp.int32, packed.shape, 1)
    return jnp.where(lane < LANES // 2, packed + pltpu.roll(packed, LANES // 2, 1), 0.0)


def put_halves(out, rel_from, rel_to, block, keep, send):
    half = len(rel_to) // 2
    at = 0
    while at < len(rel_to):
        size, start = 1, rel_from.index(rel_to[at])
        while at + size < len(rel_to) and at + size != half and start + size < len(rel_from):
            if rel_from[start + size] != rel_to[at + size]:
                break
            size += 1
        rows = out[start * block : (start + size) * block]
        if at < half:
            keep[at * block : (at + size) * block, :] = rows
        else:
            send[(at - half) * block : (at - half + size) * block, :] = rows.astype(BF16)
        at += size


def fetch_body(me_ref, *refs):
    count = (len(refs) - 2) // 2
    sources, targets, done = refs[:count], refs[count + 1 : 2 * count + 1], refs[-1]
    in_gate, forget, gain = targets[-4:-1]
    rows = gain.shape[1]
    start = pl.multiple_of(me_ref[0] * rows, rows)
    copies = []
    for i, (source, target) in enumerate(zip(sources, targets)):
        if target.shape != source.shape:
            source = source.at[:, pl.ds(start, rows)]
        copies.append(pltpu.make_async_copy(source, target, done.at[i]))
    for copy in copies:
        copy.start()
    for copy in copies:
        copy.wait()


def fetch(me, weights, in_gate, forget, gain, bias, after):
    rows, heads = weights[0].shape[0], in_gate.shape[1]
    sources = [*weights, in_gate.T, forget.T, gain[None], bias[None]]
    shapes = [w.shape for w in weights] + [(heads, rows), (heads, rows), (1, rows), (1, heads)]
    return pl.pallas_call(
        fetch_body,
        out_shape=tuple(pltpu.VMEM(shape, a.dtype) for shape, a in zip(shapes, sources)),
        in_specs=[SMEM] + [UNREAD] * len(sources) + [VMEM],
        out_specs=[VMEM] * len(sources),
        scratch_shapes=[pltpu.SemaphoreType.DMA((len(sources),))],
        compiler_params=params(4),
        name="fetch",
    )(me, *[far(a) for a in sources], near(after))


def first_body(plan, block, base_ref, *refs):
    pieces = refs[: plan.tp]
    gain_ref, w_z, w_x, w_in, w_forget = refs[plan.tp : plan.tp + 5]
    later = (len(refs) - plan.tp - 13) // 2
    refs = refs[plan.tp + 5 :]
    copies = [
        pltpu.make_async_copy(refs[i], refs[later + 5 + i], refs[-1].at[i]) for i in range(later)
    ]
    for copy in copies:
        copy.start()
    keep_z, send_z, keep_x, send_x, scaled = refs[later : later + 5]
    staged, extra = refs[-3:-1]
    cols = w_x.shape[1]
    heads = w_in.shape[0]
    for s, piece in enumerate(pieces):
        staged[s] = piece[...]
    base = base_ref[0]
    gain = gain_ref[...]
    rel = spans(plan.x_first)
    lane = lax.broadcasted_iota(jnp.int32, (block, LANES), 1)
    for i, r in enumerate(rel):
        zr, xr = r // plan.ratio, r % plan.ratio
        rows = staged[base ^ zr, pl.ds(xr * block, block), :].astype(F32)
        scaled[pl.ds(i * block, block), :] = (rows * gain).astype(BF16)
        squares = jnp.sum(rows * rows, axis=1, keepdims=True)
        extra[pl.ds(i * block, block), :] = jnp.where(lane == LANES // 2 - 1, squares, 0.0)
    half = len(rel) // 2 * block
    out = jnp.dot(scaled[...], w_z[...], preferred_element_type=F32)
    put_halves(out, rel, spans(plan.z_first), block, keep_z, send_z)
    out = jnp.dot(scaled[...], w_x[...], preferred_element_type=F32)
    keep_x[:, :cols] = out[:half]
    send_x[:, :cols] = out[half:].astype(BF16)
    dims = (((1,), (1,)), ((), ()))
    extra[:, :heads] = lax.dot_general(scaled[...], w_in[...], dims, preferred_element_type=F32)
    extra[:, heads : 2 * heads] = lax.dot_general(scaled[...], w_forget[...], dims, preferred_element_type=F32)
    keep_x[:, cols:] = extra[:half]
    send_x[:, cols:] = pack(extra[half:]).astype(BF16)
    for copy in copies:
        copy.wait()


def project_first(plan, base, pieces, gain, w_z, w_x, gate_weights, later, block):
    rows = plan.kv * block
    features, cols = w_x.shape
    half = rows // 2
    assert 2 * gate_weights[0].shape[0] < LANES // 2
    return pl.pallas_call(
        functools.partial(first_body, plan, block),
        out_shape=(
            pltpu.VMEM((half, cols), F32),
            pltpu.VMEM((half, cols), BF16),
            pltpu.VMEM((half, cols + LANES), F32),
            pltpu.VMEM((half, cols + LANES), BF16),
            pltpu.VMEM((rows, features), BF16),
        )
        + tuple(pltpu.VMEM(w.shape, BF16) for w in later),
        in_specs=[SMEM] + [VMEM] * (plan.tp + 5) + [UNREAD] * len(later),
        out_specs=[VMEM] * (5 + len(later)),
        scratch_shapes=[
            pltpu.VMEM((plan.tp, plan.ratio * block, features), BF16),
            pltpu.VMEM((rows, LANES), F32),
            pltpu.SemaphoreType.DMA((len(later),)),
        ],
        compiler_params=params(12),
        name="project_first",
    )(base, *[near(p) for p in pieces], near(gain), near(w_z), near(w_x), *[near(w) for w in gate_weights], *[far(w) for w in later])


def second_body(scaled, *refs):
    count = len(refs) // 3
    for j in range(count):
        out = jnp.dot(scaled[...], refs[j][...], preferred_element_type=F32)
        keep, send = refs[count + 2 * j], refs[count + 2 * j + 1]
        half = keep.shape[0]
        keep[...] = out[:half]
        send[...] = out[half:].astype(BF16)


def project_second(scaled, weights):
    half, cols = scaled.shape[0] // 2, weights[0].shape[1]
    return pl.pallas_call(
        second_body,
        out_shape=(pltpu.VMEM((half, cols), F32), pltpu.VMEM((half, cols), BF16)) * len(weights),
        in_specs=[VMEM] * (1 + len(weights)),
        out_specs=[VMEM] * (2 * len(weights)),
        compiler_params=params(12),
        name="project_second",
    )(near(scaled), *[near(w) for w in weights])


def step_body(plain, keep_ref, got_ref, *outs):
    keep_out, send_out = outs[-2:]
    half = keep_out.shape[0]
    keep_out[:, :plain] = keep_ref[:half, :plain] + got_ref[:half, :plain].astype(F32)
    send_out[:, :plain] = (keep_ref[half:, :plain] + got_ref[half:, :plain].astype(F32)).astype(BF16)
    if plain < keep_ref.shape[1]:
        sums = keep_ref[:, plain:] + unpack(got_ref[:, plain:].astype(F32))
        keep_out[:, plain:] = sums[:half]
        send_out[:, plain:] = pack(sums[half:]).astype(BF16)


def reduce_step(plain, keep, got, *after):
    half, wide = keep.shape[0] // 2, keep.shape[1]
    return pl.pallas_call(
        functools.partial(step_body, plain),
        out_shape=(pltpu.VMEM((half, wide), F32), pltpu.VMEM((half, wide), BF16)),
        in_specs=[VMEM] * (2 + len(after)),
        out_specs=[VMEM] * 2,
        compiler_params=params(4),
        name="reduce_step",
    )(near(keep), near(got), *[near(a) for a in after])


def state_body(
    first, taken_ref, stab_ref, memory_ref, norm_ref, in_ref, forget_ref, key_ref, value_ref, later_ref, *refs
):
    new_ref, new_norm, narrow_ref, narrow_norm, stable_ref, rows_ref, later_out = refs[-18:-11]
    memory, gained, norm, past_in, past_forget, keys, values, small, got, put, put_norm = refs[-11:]
    size, heads, dk = norm.shape
    chain, seqs = past_in.shape[0], past_in.shape[2]
    mine = pl.ds(first, size)
    loads = [
        pltpu.make_async_copy(source, target, small.at[i])
        for i, (source, target) in enumerate(
            (
                (in_ref, past_in),
                (forget_ref, past_forget),
                (key_ref.at[mine], keys),
                (value_ref.at[mine], values),
                (norm_ref.at[mine], norm),
            )
        )
    ]
    reads = [pltpu.make_async_copy(memory_ref.at[first + i], memory.at[i], got.at[i]) for i in range(size)]
    writes = [pltpu.make_async_copy(memory.at[i], new_ref.at[first + i], put.at[i]) for i in range(size)]
    share_rows = later_out.shape[0]
    at = pl.ds(first // size * share_rows, share_rows)
    writes.append(pltpu.make_async_copy(later_ref.at[at], later_out, small.at[5]))
    for copy in loads + reads + writes[size:]:
        copy.start()
    for copy in loads:
        copy.wait()
    count = taken_ref[...]
    total = jnp.zeros((heads, seqs), F32)
    runs, ends, share = [], [], []
    for j in range(chain):
        total = total + jnp.where(j < count, jax.nn.log_sigmoid(past_forget[j]), 0.0)
        runs.append(total)
    carried = total + stab_ref[...]
    stable = carried
    for j in range(chain):
        ends.append(jnp.where(j < count, total - runs[j] + past_in[j], -jnp.inf))
        stable = jnp.maximum(stable, ends[j])
    stable_ref[...] = stable
    tall = jnp.concatenate([stable, jnp.zeros((LANES - heads, seqs), F32)], axis=0)
    tall = jnp.concatenate([tall, jnp.zeros((LANES, LANES - seqs), F32)], axis=1)
    rows_ref[...] = tall.T[:seqs, :]
    decay = jnp.exp(carried - stable)
    for j in range(chain):
        share.append(jnp.exp(ends[j] - stable) * dk**-0.5)
    for i, h in [(i, h) for i in range(size) for h in range(heads)]:
        a, b, s = h * dk, (h + 1) * dk, first + i
        key_rows = keys[i, :, a:b].astype(F32)
        value_rows = values[i, :, a:b].astype(F32)
        weighted = jnp.concatenate(
            [key_rows[j : j + 1] * share[j][h : h + 1, s : s + 1] for j in range(chain)], axis=0
        )
        high = weighted.astype(BF16).astype(F32)
        pair = jnp.concatenate([high, weighted - high], axis=0).astype(BF16)
        twice = jnp.concatenate([value_rows, value_rows], axis=0).astype(BF16)
        gained[i, h] = lax.dot_general(pair, twice, (((0,), (0,)), ((), ())), preferred_element_type=F32)
        line = decay[h : h + 1, s : s + 1] * norm[i, h : h + 1, :] + jnp.sum(weighted, axis=0, keepdims=True)
        norm[i, h : h + 1, :] = line
        narrow_norm[i : i + 1, a:b] = line
    for i in range(size):
        reads[i].wait()
        for h in range(heads):
            fresh = decay[h : h + 1, first + i : first + i + 1] * memory[i, h] + gained[i, h]
            memory[i, h] = fresh
            narrow_ref[i, h] = fresh.astype(BF16)
        writes[i].start()
    last = pltpu.make_async_copy(norm, new_norm.at[mine], put_norm)
    last.start()
    for copy in writes + [last]:
        copy.wait()


def state_update(part, parts, taken, memory, norm, stab, past_in, past_forget, keys, values, later, previous, after):
    seqs, heads, dk, dv = memory.shape
    chain = past_in.shape[1]
    size = seqs // parts
    assert heads <= 8 and seqs <= 8
    inputs = [memory, norm, past_in.transpose(1, 2, 0), past_forget.transpose(1, 2, 0), keys, values, later]
    return pl.pallas_call(
        functools.partial(state_body, part * size),
        out_shape=(
            pltpu.HBM(memory.shape, F32),
            pltpu.HBM(norm.shape, F32),
            pltpu.VMEM((size, heads, dk, dv), BF16),
            pltpu.VMEM((size, heads * dk), F32),
            pltpu.VMEM((heads, seqs), F32),
            pltpu.VMEM((seqs, LANES), F32),
            pltpu.VMEM((later.shape[0] // parts, later.shape[1]), later.dtype),
        ),
        in_specs=[VMEM, VMEM] + [UNREAD] * len(inputs) + [VMEM] + [UNREAD] * len(previous),
        out_specs=[UNREAD, UNREAD] + [VMEM] * 5,
        input_output_aliases={10 + i: i for i in range(len(previous))},
        scratch_shapes=[
            pltpu.VMEM((size, heads, dk, dv), F32),
            pltpu.VMEM((size, heads, dk, dv), F32),
            pltpu.VMEM((size, heads, dk), F32),
            pltpu.VMEM((chain, heads, seqs), F32),
            pltpu.VMEM((chain, heads, seqs), F32),
            pltpu.VMEM((size,) + keys.shape[1:], BF16),
            pltpu.VMEM((size,) + values.shape[1:], BF16),
            pltpu.SemaphoreType.DMA((6,)),
            pltpu.SemaphoreType.DMA((size,)),
            pltpu.SemaphoreType.DMA((size,)),
            pltpu.SemaphoreType.DMA(()),
        ],
        cost_estimate=pl.CostEstimate(
            flops=16 * memory.size // parts, bytes_accessed=8 * memory.size // parts, transcendentals=0
        ),
        compiler_params=params(14),
        name="state_update",
    )(taken[None], stab.T, *[far(a) for a in inputs], near(after), *[far(a) for a in previous])


def advance_body(
    width, chain, heads, keep_q, got_q, keep_k, got_k, keep_v, got_v, keep_o, got_o, mine_ref, stab_ref, bias_ref, *refs
):
    parts = (len(refs) - 3) // 2
    memories, norms = refs[:parts], refs[parts : 2 * parts]
    gated, key_out, value_out = refs[2 * parts :]
    rows = keep_q.shape[0]
    cols = gated.shape[1]
    all_heads = bias_ref.shape[1]
    each = memories[0].shape[0]
    dk = cols // heads
    extra = keep_q[:, cols:] + unpack(got_q[:, cols:].astype(F32))
    scale = lax.rsqrt(extra[:, LANES // 2 - 1 : LANES // 2] / width + EPSILON)
    gates = extra * scale
    mine = mine_ref[0] * heads
    in_gate = pltpu.roll(gates, LANES - mine, 1)
    bias = jnp.concatenate([bias_ref[...], jnp.zeros((1, LANES - all_heads), F32)], axis=1)
    pre = pltpu.roll(pltpu.roll(gates, LANES - all_heads, 1) + bias, LANES - mine, 1)
    stab = jnp.zeros((rows, LANES), F32)
    stab_row = lax.broadcasted_iota(jnp.int32, (rows, LANES), 0) // chain
    for s in range(rows // chain):
        stab = jnp.where(stab_row == s, stab_ref[s : s + 1, :], stab)
    log_f = jax.nn.log_sigmoid(pre)
    turn = lax.broadcasted_iota(jnp.int32, (rows, LANES), 0) % chain
    running = log_f
    shift = 1
    while shift < chain:
        running = running + jnp.where(turn >= shift, pltpu.roll(running, shift, 0), 0.0)
        shift *= 2
    fresh = in_gate - running
    best = fresh
    shift = 1
    while shift < chain:
        best = jnp.maximum(best, jnp.where(turn >= shift, pltpu.roll(best, shift, 0), -jnp.inf))
        shift *= 2
    carried = running + stab
    stable = jnp.maximum(carried, running + best)
    carry_weight = jnp.exp(carried - stable)
    lead = running - stable
    fresh_t = fresh.T
    at_t = lax.broadcasted_iota(jnp.int32, (rows, rows), 0)
    at_s = lax.broadcasted_iota(jnp.int32, (rows, rows), 1)
    seen = (at_t // chain == at_s // chain) & (at_s <= at_t)
    seqs = rows // chain
    seq_t = lax.broadcasted_iota(jnp.int32, (rows, seqs), 0) // chain
    seq_s = lax.broadcasted_iota(jnp.int32, (rows, seqs), 1)
    sub = 8
    sub_row = lax.broadcasted_iota(jnp.int32, (sub, dk), 0) // chain
    for h in range(heads):
        a, b = h * dk, (h + 1) * dk

        def total(keep, got):
            return ((keep[:, a:b] + got[:, a:b].astype(F32)) * scale).astype(BF16)

        query, key, value = total(keep_q, got_q), total(keep_k, got_k), total(keep_v, got_v)
        gate = total(keep_o, got_o).astype(F32)
        key_out[:, a:b] = key
        value_out[:, a:b] = value
        scores = lax.dot_general(query, key, (((1,), (1,)), ((), ())), preferred_element_type=F32)
        weight = jnp.exp(jnp.where(seen, lead[:, h : h + 1] + fresh_t[h : h + 1, :], -jnp.inf))
        scores = scores * (weight * dk**-0.5)
        carry = carry_weight[:, h : h + 1]
        high = scores.astype(BF16)
        low = (scores - high.astype(F32)).astype(BF16)
        inner = jnp.dot(high, value, preferred_element_type=F32) + jnp.dot(
            low, value, preferred_element_type=F32
        )
        normal = jnp.concatenate([norm[:, a:b] for norm in norms], axis=0)
        n_high = normal.astype(BF16)
        n_low = (normal - n_high.astype(F32)).astype(BF16)
        dims = (((1,), (1,)), ((), ()))
        along = lax.dot_general(query, n_high, dims, preferred_element_type=F32) + lax.dot_general(
            query, n_low, dims, preferred_element_type=F32
        )
        along = jnp.sum(jnp.where(seq_t == seq_s, along, 0.0), axis=1, keepdims=True)
        below = carry * along + jnp.sum(scores, axis=1, keepdims=True)
        parts = []
        for r in range(0, rows, sub):
            part = None
            for i in range(sub // chain):
                s = r // chain + i
                one = jnp.dot(
                    query[r : r + sub], memories[s // each][s % each, h], preferred_element_type=F32
                )
                part = one if part is None else jnp.where(sub_row == i, one, part)
            parts.append(part)
        outer = jnp.concatenate(parts, axis=0)
        hidden = (carry * outer + inner) / jnp.maximum(jnp.abs(below), 1.0)
        gated[:, a:b] = (jax.nn.sigmoid(gate) * hidden).astype(BF16)


def advance(width, chain, heads, mine, sums, memories, norms, stab, bias):
    rows, cols = sums[-1].shape
    parts = len(memories)
    return pl.pallas_call(
        functools.partial(advance_body, width, chain, heads),
        out_shape=(
            pltpu.VMEM((rows, cols), BF16),
            jax.ShapeDtypeStruct((rows, cols), BF16),
            jax.ShapeDtypeStruct((rows, cols), BF16),
        ),
        in_specs=[VMEM] * 8 + [SMEM, VMEM, VMEM] + [VMEM] * (2 * parts),
        out_specs=[VMEM] * 3,
        compiler_params=params(12),
        name="advance",
    )(*[near(a) for a in sums], mine, near(stab), near(bias), *[near(m) for m in memories], *[near(n) for n in norms])


def output_body(plan, block, base_ref, *refs):
    pieces, weights = refs[: plan.kv], refs[plan.kv : -3]
    keep, send, staged = refs[-3:]
    r, t = plan.ratio, plan.tp
    for rel, piece in enumerate(pieces):
        staged[rel // r, (rel % r) * block : (rel % r + 1) * block, :] = piece[...]
    base = base_ref[0]
    rows = jnp.concatenate([staged[base ^ s] for s in spans(masks_of(t))], axis=0)
    share = weights[0].shape[0]
    out = jnp.dot(rows[:, :share], weights[0][...], preferred_element_type=F32)
    for i in range(1, len(weights)):
        out = out + jnp.dot(rows[:, i * share : (i + 1) * share], weights[i][...], preferred_element_type=F32)
    cut = t // 2 * r * block
    keep[...] = out[:cut]
    send[...] = out[cut:].astype(BF16)


def output_product(plan, base, pieces, weights, block):
    rows = plan.kv * block // 2
    cols = weights[0].shape[1]
    return pl.pallas_call(
        functools.partial(output_body, plan, block),
        out_shape=(pltpu.VMEM((rows, cols), F32), pltpu.VMEM((rows, cols), BF16)),
        in_specs=[SMEM] + [VMEM] * (plan.kv + len(weights)),
        out_specs=[VMEM] * 2,
        scratch_shapes=[pltpu.VMEM((plan.tp, plan.ratio * block, pieces[0].shape[1]), BF16)],
        compiler_params=params(8),
        name="output_product",
    )(base, *[near(p) for p in pieces], *[near(w) for w in weights])


def gather_route(plan):
    bits = plan.tp.bit_length() - 1
    z, x = plan.z_first[:bits], plan.z_first[bits:]
    if len(z) == 2 and len(x) == 1:
        near_z, over_z, x = z[0], z[1], x[0]
        return [
            (over_z, 0, over_z),
            (near_z, 0, near_z),
            (x, 0, x),
            (near_z ^ over_z, over_z, near_z),
            (near_z ^ x, near_z, x),
            (over_z ^ x, over_z, x),
            (near_z ^ over_z ^ x, over_z ^ x, near_z),
        ]
    route, held = [], [0]
    for mask in z[::-1] + x:
        route += [(block ^ mask, block, mask) for block in held]
        held += [block ^ mask for block in held]
    return route


def body(
    plan,
    tokens,
    norm_gain,
    query_weight,
    key_weight,
    value_weight,
    outgate_weight,
    ingate_weight,
    forget_weight,
    forget_bias,
    output_weight,
    state_memory,
    state_normaliser,
    state_stabiliser,
    past_keys,
    past_values,
    past_ingate,
    past_forget,
    accepted,
):
    seqs, heads = state_stabiliser.shape
    block, part = tokens.shape
    chain = past_keys.shape[1]
    features = query_weight.shape[0]
    width = norm_gain.shape[0]
    ratio, tp = plan.ratio, plan.tp
    me, mine = lax.axis_index("kv"), lax.axis_index("tp")
    z, x = me // ratio, me % ratio
    me_at, base, mine_at = (v.astype(jnp.int32)[None] for v in (me, z ^ mine, mine))

    def pull(array, pairs):
        return lax.ppermute(array, BOTH, pairs)

    cuts = [lax.dynamic_slice_in_dim(tokens, (x ^ m) * features, features, 1) for m in range(ratio)]
    own = jnp.concatenate([pull(cut, plan.swap(m)) for m, cut in enumerate(cuts)], axis=0)
    w_o, w_q, w_in, w_forget, gain, bias = fetch(
        me_at, (outgate_weight, query_weight), ingate_weight, forget_weight, norm_gain, forget_bias, cuts[-1]
    )
    pieces = [own] + [pull(own, plan.xor_tp(s)) for s in range(1, tp)]

    keep_o, send_o, keep_q, send_q, scaled, w_k, w_v = project_first(
        plan, base, pieces, gain, w_o, w_q, (w_in, w_forget), (key_weight, value_weight), block
    )
    keep_k, send_k, keep_v, send_v = project_second(scaled, (w_k, w_v))
    cols = query_weight.shape[1]
    steps = len(plan.x_first)
    sums = [keep_q, send_q, keep_k, send_k, keep_v, send_v, keep_o, send_o]
    orders = [plan.x_first] * 3 + [plan.z_first]
    parts = 2 if seqs % 2 == 0 else 1
    states, previous, after = [], (), send_v
    for i in range(steps):
        for j, order in zip((0, 3, 1, 2), (orders[n] for n in (0, 3, 1, 2))):
            got = pull(sums[2 * j + 1], plan.xor_kv(order[i]))
            if i + 1 < steps:
                wait = ()
                if len(states) < parts and (i, j) in ((0, 0), (0, 1)):
                    states.append(
                        state_update(
                            len(states), parts, accepted, state_memory, state_normaliser, state_stabiliser,
                            past_ingate, past_forget, past_keys, past_values, output_weight, previous, after,
                        )
                    )
                    previous = states[-1][:2]
                    wait = (states[-1][3],)
                sums[2 * j], sums[2 * j + 1] = reduce_step(cols, sums[2 * j], got, *wait)
                after = sums[2 * j + 1]
            else:
                sums[2 * j + 1] = got
    memory, normaliser = previous
    stable = states[0][4].T

    gated, new_keys, new_values = advance(
        width, chain, heads, mine_at, sums, [a[2] for a in states], [a[3] for a in states], states[0][5], bias
    )

    held = {0: gated}
    for wanted, source, mask in gather_route(plan):
        held[wanted] = pull(held[source], plan.xor_kv(mask))
    keep, send = output_product(plan, base, [held[m] for m in range(plan.kv)], [a[6] for a in states], block)
    masks = masks_of(tp)
    for mask in masks[:-1]:
        keep, send = reduce_step(keep.shape[1], keep, pull(send, plan.xor_tp(mask)))
    total = (keep + pull(send, plan.xor_tp(masks[-1])).astype(F32)).astype(BF16)
    back = [pull(total[m * block : (m + 1) * block], plan.swap(m)) for m in range(ratio)]
    stacked = jnp.stack(back, axis=0)
    mixed = jnp.concatenate(
        [lax.dynamic_index_in_dim(stacked, x ^ m, 0, keepdims=False) for m in range(ratio)], axis=1
    )
    return (mixed, memory, normaliser, stable, new_keys, new_values)


def solution(mesh):
    placed = (
        P("kv", "tp"),
        P(),
        P("kv", "tp"),
        P("kv", "tp"),
        P("kv", "tp"),
        P("kv", "tp"),
        P(),
        P(),
        P(),
        P("tp", "kv"),
        P("kv", "tp", None, None),
        P("kv", "tp", None),
        P("kv", "tp"),
        P("kv", None, "tp"),
        P("kv", None, "tp"),
        P("kv", None, "tp"),
        P("kv", None, "tp"),
        P("kv"),
    )
    return jax.shard_map(
        functools.partial(body, Plan(mesh)),
        mesh=mesh,
        in_specs=placed,
        out_specs=(
            P("kv", "tp"),
            P("kv", "tp", None, None),
            P("kv", "tp", None),
            P("kv", "tp"),
            P("kv", "tp"),
            P("kv", "tp"),
        ),
        check_vma=False,
    )
```
